32 devices in a mesh: fs: 8 (over z, y), tp: 4 (over x, core).
Axes of the slice: x: 2, y: 2, z: 4, core: 2. Of those that a mesh axis runs over, the one named last changes fastest.
Arguments:
- tokens: bfloat16 [3072, 2048], P('tp'), may hold values from -6 to 6
- norm_gain: float32 [2048], P('fs'), may hold values from 0.1 to 1.9
- gate_weight: float32 [4, 2048, 8192], P(None, 'fs', 'tp'), may hold values from -0.125 to 0.125
- up_weight: float32 [4, 2048, 8192], P(None, 'fs', 'tp'), may hold values from -0.125 to 0.125
- down_weight: float32 [4, 8192, 2048], P(None, 'fs', 'tp'), may hold values from -0.0625 to 0.0625
- routes: int32 [3072, 2], P('tp'), may hold values from 0 to 3, all different within a row; in each aligned block of 768 rows (0 to 767, 768 to 1535, ...) at most 480 rows name the same one
- route_logit: float32 [3072, 2], P('tp'), may hold values from -6 to 6
Outputs:
- gate_out: bfloat16 [4, 2048, 8192], P(None, None, 'fs')
- up_out: bfloat16 [4, 2048, 8192], P(None, None, 'fs')
- down_out: bfloat16 [4, 8192, 2048], P(None, 'fs')
- mixed: bfloat16 [3072, 2048], P(('tp', 'fs'))
The draws below stay inside these ranges and needn't reach their ends.
Inputs may be any that keep to these rules, and one draw needn't show every extreme that they name: `routes`: the two experts of a token differ. In each aligned block of 768 tokens (the tokens of one request group) every expert is named by at most 480 tokens, a bound that some block reaches.
All inputs are finite; a program needn't handle non-finite values.
Results may differ from the reference program's by a relative error of at most 0.0082.
Values may be sent and summed in bfloat16 or wider, within the bound.
No kernel may reach another device: no remote copies, remote signals or barrier semaphores. Data moves between devices by JAX's collectives and lax.ppermute only.
A program may use at most 192 MiB of HBM per device.

```python
import math
import jax
import jax.numpy as jnp
import numpy as np
from jax import lax

D = 2048
FF = 8192
E = 4
TOK_GROUP = 768
CAP = 480
TOKENS = 3072


def levels(stream_key, dims, shards, least, largest):
    factor_of = 1.0
    for axis_at, parts in shards:
        steps = jax.random.uniform(jax.random.fold_in(jax.random.fold_in(stream_key, 6), axis_at), (parts,), jnp.float32, least / len(shards), largest / len(shards))
        factor_of = factor_of * jnp.repeat(jnp.exp(steps), dims[axis_at] // parts).reshape((-1,) + (1,) * (len(dims) - 1 - axis_at))
    return factor_of


def deal_out(rng, own, number, rows, number_of, top, limit, skew):
    sequence = jax.random.permutation(rng, number_of)
    packed, ordinary = load_shares(number_of, rows * top, limit, skew, True), load_shares(number_of, rows * top, limit, skew, False)
    places = jnp.arange(number_of)

    def named(tallies, rotation):
        used = int((tallies > 0).sum())
        fixed = max(1, used // 4)
        passed = fixed + (places - fixed + rotation * (used - fixed)) % max(1, number_of - fixed)
        return jnp.zeros((number_of,), jnp.int32).at[sequence[jnp.where(places < fixed, places, passed)]].set(jnp.asarray(tallies, jnp.int32))

    tallies = jnp.where(number % 4 == 0, named(packed, number // 4), named(ordinary, number - number // 4 - 1))
    mixed = jax.random.permutation(jax.random.fold_in(own, 3), number_of)
    source_of, receiver = mixed[0:number_of // 2 * 2:2], mixed[1:number_of // 2 * 2:2]
    margin = jnp.minimum(tallies[source_of] - 1, limit - tallies[receiver]) // 2
    margin = jnp.where((source_of == sequence[0]) | (receiver == sequence[0]) | (tallies[receiver] == 0), 0, jnp.maximum(margin, 0))
    passed = jax.random.randint(jax.random.fold_in(own, 4), (number_of // 2,), 0, 1 << 20) % (margin + 1)
    tallies = tallies.at[source_of].add(-passed).at[receiver].add(passed)
    items = jnp.searchsorted(jnp.cumsum(tallies), jnp.arange(rows * top), side="right").astype(jnp.int32)
    grid = items.reshape(top, rows).T
    grid = grid[jax.random.permutation(jax.random.fold_in(own, 1), rows)]
    rotation = jax.random.randint(jax.random.fold_in(own, 2), (rows, 1), 0, top)
    return jnp.take_along_axis(grid, (jnp.arange(top)[None, :] + rotation) % top, axis=1)


def load_shares(amount, total, bound, skew, full):
    loads = [(1 << 20) // math.isqrt(grade ** skew) + 1 for grade in range(1, amount + 1)]
    largest = bound if full else min(bound, max(-(-total // amount), total * loads[0] // sum(loads)))
    least = 1 if total - largest >= amount - 1 else 0
    counts, spare = [largest] + [least] * (amount - 1), total - largest - least * (amount - 1)
    while spare > 0:
        movable = [i for i in range(1, amount) if counts[i] < largest] or [i for i in range(1, amount) if counts[i] < bound]
        pool, left = sum([loads[i] for i in movable]), spare
        for i in movable:
            more = min(bound - counts[i], max(1, left * loads[i] // pool), spare)
            counts[i] = counts[i] + more
            spare = spare - more
    return np.array(counts)


def scatter_about(stream_key, shape, deviation, limit, pieces=(), held_as=jnp.bfloat16):
    entries = jax.random.normal(stream_key, shape, jnp.float32) * deviation
    if len(pieces) > 0:
        entries = levels(stream_key, shape, pieces, -0.22, 0.18) * entries
    return jnp.clip(entries, min=-limit, max=limit).astype(held_as)


def setup_inputs(seed: int = 0) -> dict:
    seeds = jax.random.split(jax.random.key(seed), 8)
    tokens = scatter_about(seeds[0], (TOKENS, D), 1.0, 6.0, ((0, 4),))
    norm_gain = jnp.clip(1.0 + 0.18 * jax.random.normal(seeds[1], (D,), jnp.float32), 0.1, 1.9)
    gate_weight = scatter_about(seeds[2], (E, D, FF), D ** -0.5, 0.125, ((1, 8), (2, 4)), jnp.float32)
    up_weight = scatter_about(seeds[3], (E, D, FF), D ** -0.5, 0.125, ((1, 8), (2, 4)), jnp.float32)
    down_weight = scatter_about(seeds[4], (E, FF, D), FF ** -0.5, 0.0625, ((1, 8), (2, 4)), jnp.float32)
    routes_keys = jax.random.split(jax.random.fold_in(seeds[5], 1), TOKENS // TOK_GROUP)
    routes_turns = jax.random.permutation(jax.random.fold_in(seeds[5], 3), TOKENS // TOK_GROUP)
    routes = jax.vmap(lambda own, number: deal_out(jax.random.fold_in(seeds[5], 2), own, number, TOK_GROUP, E, 2, CAP, 1))(routes_keys, routes_turns).reshape((TOKENS, 2))
    route_logit = scatter_about(seeds[6], (TOKENS, 2), 1.0, 6.0, ((0, 4),), jnp.float32)
    return dict(tokens=tokens, norm_gain=norm_gain, gate_weight=gate_weight, up_weight=up_weight, down_weight=down_weight, routes=routes, route_logit=route_logit)


EPS = 0.5

def reference(tokens, norm_gain, gate_weight, up_weight, down_weight, routes, route_logit):
    gain_col = norm_gain.astype(jnp.float32)[None, :, None]
    gate_out = (gate_weight * gain_col).astype(jnp.bfloat16)
    up_out = (up_weight * gain_col).astype(jnp.bfloat16)
    down_out = down_weight.astype(jnp.bfloat16)
    floats = tokens.astype(jnp.float32)
    normed = (floats * lax.rsqrt(lax.optimization_barrier(jnp.mean(floats * floats, axis=1, keepdims=True)) + EPS)).astype(jnp.bfloat16)
    first_share = jax.nn.sigmoid(route_logit[:, 0] - route_logit[:, 1])
    shares = jnp.stack([first_share, 1.0 - first_share], axis=1)
    summed = jnp.zeros(tokens.shape, jnp.float32)
    for expert in range(E):
        weight_col = lax.optimization_barrier(jnp.sum(jnp.where(routes == expert, shares, 0.0), axis=1, keepdims=True))
        gate_val = jnp.dot(normed, gate_out[expert], preferred_element_type=jnp.float32)
        up_val = jnp.dot(normed, up_out[expert], preferred_element_type=jnp.float32)
        hidden = (jax.nn.silu(gate_val) * up_val).astype(jnp.bfloat16)
        result = jnp.dot(hidden, down_out[expert], preferred_element_type=jnp.float32)
        summed = summed + weight_col * result
    return (gate_out, up_out, down_out, summed.astype(jnp.bfloat16))
```

```python
import functools

import jax
import jax.numpy as jnp
from jax import lax
from jax.experimental import pallas as pl
from jax.experimental.pallas import tpu as pltpu
from jax.sharding import PartitionSpec as P


EPS = 0.5
ANY = pl.BlockSpec(memory_space=pl.ANY)
SMEM = pl.BlockSpec(memory_space=pltpu.SMEM)
VMEM = pl.BlockSpec(memory_space=pltpu.VMEM)


def cast_whole(gate_ref, up_ref, gain_ref, own_ref):
    gain = gain_ref[...]
    own_ref[0, 0] = (gate_ref[0] * gain).astype(jnp.bfloat16)
    own_ref[0, 1] = (up_ref[0] * gain).astype(jnp.bfloat16)


def cast_halves(where_ref, gate_ref, up_ref, gain_ref, keep_ref, send_ref):
    half = keep_ref.shape[2]
    x = where_ref[0]
    for out_ref, at in ((keep_ref, x), (send_ref, 1 - x)):
        rows = pl.ds(pl.multiple_of(at * half, half), half)
        gain = gain_ref[rows, :]
        out_ref[0, 0] = (gate_ref[0, rows, :] * gain).astype(jnp.bfloat16)
        out_ref[0, 1] = (up_ref[0, rows, :] * gain).astype(jnp.bfloat16)


def cast(gate_weight, up_weight, gain_col, where, expert, halves):
    _, rows, cols = gate_weight.shape
    wide = cols // 2
    weight_spec = pl.BlockSpec((1, rows, wide), lambda i: (expert, 0, i))
    gain_spec = pl.BlockSpec((rows, 1), lambda i: (0, 0))
    if not halves:
        return pl.pallas_call(
            cast_whole,
            grid=(2,),
            in_specs=[weight_spec, weight_spec, gain_spec],
            out_specs=pl.BlockSpec((1, 2, rows, wide), lambda i: (i, 0, 0, 0)),
            out_shape=jax.ShapeDtypeStruct((2, 2, rows, wide), jnp.bfloat16),
        )(gate_weight, up_weight, gain_col)
    out_spec = pl.BlockSpec((1, 2, rows // 2, wide), lambda i: (i, 0, 0, 0))
    out = jax.ShapeDtypeStruct((2, 2, rows // 2, wide), jnp.bfloat16)
    return pl.pallas_call(
        cast_halves,
        grid=(2,),
        in_specs=[SMEM, weight_spec, weight_spec, gain_spec],
        out_specs=[out_spec, out_spec],
        out_shape=[out, out],
    )(where, gate_weight, up_weight, gain_col)


def pick_kernel(where_ref, own_ref, got_ref, *outs):
    flag, y = where_ref[1], where_ref[2]
    for r in range(2):
        at = y if r == 0 else 1 - y

        @pl.when(flag == 0)
        def _():
            outs[r][...] = own_ref[at]
            outs[2 + r][...] = got_ref[at]

        @pl.when(flag != 0)
        def _():
            outs[r][...] = got_ref[at]
            outs[2 + r][...] = own_ref[at]


def pick(where, own, got):
    sides, kinds, rows, wide = own.shape
    block = min(128, rows)
    in_spec = pl.BlockSpec((sides, 1, block, wide), lambda i, j: (0, i, j, 0))
    out_spec = pl.BlockSpec((1, block, wide), lambda i, j: (i, j, 0))
    out = jax.ShapeDtypeStruct(own.shape[1:], own.dtype)
    return pl.pallas_call(
        pick_kernel,
        grid=(kinds, rows // block),
        in_specs=[SMEM, in_spec, in_spec],
        out_specs=[out_spec] * 4,
        out_shape=[out] * 4,
    )(where, own, got)


def expert_kernel(
    where_ref, share_ref, normed_ref, *refs, expert, sizes, has_outs, has_acc, last, parts
):
    rows_in, pieces_n, downs_n = sizes
    pieces, refs = refs[:pieces_n], refs[pieces_n:]
    downs, refs = refs[:downs_n], refs[downs_n:]
    if has_outs:
        refs = refs[3:]
    if has_acc:
        acc_in, refs = refs[0], refs[1:]
    (gate_out, up_out, down_out), refs = refs[:3], refs[3:]
    if last:
        final_refs, refs = refs[:parts], refs[parts:]
    else:
        acc_out, refs = refs[0], refs[1:]
    gate_v, up_v, down_v, hidden_v, acc_v, in_sem, down_sem, out_sem, acc_sem = refs
    base, x, tp, fs = where_ref[3], where_ref[0], where_ref[4], where_ref[5]
    copies = [[], []]
    for i in range(pieces_n):
        if pieces_n == parts:
            at = (base ^ i) * rows_in
        else:
            at = (base ^ (i // 2)) * (2 * rows_in) + (x ^ (i % 2)) * rows_in
        rows = pl.ds(pl.multiple_of(at, rows_in), rows_in)
        for kind, to in ((0, gate_v), (1, up_v)):
            copies[kind].append(
                pltpu.make_async_copy(
                    pieces[i].at[kind], to.at[rows, :], in_sem.at[kind, i]
                )
            )
    for kind in range(2):
        for item in copies[kind]:
            item.start()
    wide = downs[0].shape[1]
    down_copies = []
    for i in range(downs_n):
        cols = pl.ds(pl.multiple_of((tp ^ i) * wide, wide), wide)
        item = pltpu.make_async_copy(downs[i], down_v.at[:, cols], down_sem.at[i])
        item.start()
        down_copies.append(item)
    if has_acc:
        acc_copy = pltpu.make_async_copy(acc_in, acc_v, acc_sem.at[0])
        acc_copy.start()
    leaves = [
        pltpu.make_async_copy(gate_v, gate_out.at[expert], out_sem.at[0]),
        pltpu.make_async_copy(up_v, up_out.at[expert], out_sem.at[1]),
        pltpu.make_async_copy(down_v, down_out.at[expert], out_sem.at[2]),
    ]
    for kind in range(2):
        for item in copies[kind]:
            item.wait()
        leaves[kind].start()
    tokens = normed_ref.shape[0]
    units = gate_v.shape[1]
    step = min(256, units)
    for n in range(units // step):
        cols = slice(n * step, (n + 1) * step)
        gate_val = jnp.dot(normed_ref[...], gate_v[:, cols], preferred_element_type=jnp.float32)
        up_val = jnp.dot(normed_ref[...], up_v[:, cols], preferred_element_type=jnp.float32)
        hidden_v[:, cols] = (gate_val / (1.0 + jnp.exp(-gate_val)) * up_val).astype(jnp.bfloat16)
    for item in down_copies:
        item.wait()
    leaves[2].start()
    if has_acc:
        acc_copy.wait()
    width = down_v.shape[1]
    step = min(512, width)
    share = share_ref[...]
    for n in range(width // step):
        cols = slice(n * step, (n + 1) * step)
        result = share * jnp.dot(
            hidden_v[...], down_v[:, cols], preferred_element_type=jnp.float32
        )
        acc_v[:, cols] = acc_v[:, cols] + result if has_acc else result
    if last:
        block = tokens // parts
        for i in range(parts):
            rows = pl.ds(pl.multiple_of((fs ^ i) * block, block), block)
            final_refs[i][...] = acc_v[rows, :].astype(final_refs[i].dtype)
    else:
        acc_copy = pltpu.make_async_copy(acc_v, acc_out, acc_sem.at[0])
        acc_copy.start()
        acc_copy.wait()
    for item in leaves:
        item.wait()


def expert_step(where, share, normed, pieces, downs, outs, acc, expert, experts, last, parts):
    tokens, width = normed.shape
    rows_in, units = pieces[0].shape[1:]
    fan = downs[0].shape[0]
    sizes = (rows_in, len(pieces), len(downs))
    operands = [where, share, normed, *pieces, *downs]
    specs = [SMEM, VMEM, VMEM] + [ANY] * (len(pieces) + len(downs))
    aliases = {}
    if outs is not None:
        for i in range(3):
            aliases[len(operands) + i] = i
        operands += list(outs)
        specs += [ANY] * 3
    if acc is not None:
        operands.append(acc)
        specs.append(ANY)
    shapes = [
        jax.ShapeDtypeStruct((experts, width, units), jnp.bfloat16),
        jax.ShapeDtypeStruct((experts, width, units), jnp.bfloat16),
        jax.ShapeDtypeStruct((experts, fan, width), jnp.bfloat16),
    ]
    out_specs = [ANY] * 3
    if last:
        block = tokens // parts
        for i in range(parts):
            shapes.append(
                jax.ShapeDtypeStruct((block, width), jnp.float32 if i == 0 else jnp.bfloat16)
            )
        out_specs += [VMEM] * parts
    else:
        shapes.append(jax.ShapeDtypeStruct((tokens, width), jnp.float32))
        out_specs.append(ANY)
    body = functools.partial(
        expert_kernel,
        expert=expert,
        sizes=sizes,
        has_outs=outs is not None,
        has_acc=acc is not None,
        last=last,
        parts=parts,
    )
    flops = 6 * tokens * width * units
    return pl.pallas_call(
        body,
        in_specs=specs,
        out_specs=out_specs,
        out_shape=shapes,
        input_output_aliases=aliases,
        scratch_shapes=[
            pltpu.VMEM((width, units), jnp.bfloat16),
            pltpu.VMEM((width, units), jnp.bfloat16),
            pltpu.VMEM((fan, width), jnp.bfloat16),
            pltpu.VMEM((tokens, units), jnp.bfloat16),
            pltpu.VMEM((tokens, width), jnp.float32),
            pltpu.SemaphoreType.DMA((2, len(pieces))),
            pltpu.SemaphoreType.DMA((len(downs),)),
            pltpu.SemaphoreType.DMA((3,)),
            pltpu.SemaphoreType.DMA((1,)),
        ],
        compiler_params=pltpu.CompilerParams(vmem_limit_bytes=56 * 1024 * 1024),
        cost_estimate=pl.CostEstimate(
            flops=flops, transcendentals=tokens * units, bytes_accessed=6 * width * units
        ),
    )(*operands)


def make_fast(fs_size, tp_size):
    def table(target):
        pairs = []
        for f in range(fs_size):
            for t in range(tp_size):
                to_f, to_t = target(f, t)
                pairs.append((f * tp_size + t, to_f * tp_size + to_t))
        return pairs

    across_x = table(lambda f, t: (f, t ^ 2))
    across_core = table(lambda f, t: (f, t ^ 1))
    plane = [
        table(
            lambda f, t, a=a, r=r: (
                ((f >> 2) ^ a) << 2 | (t & 1) << 1 | ((f & 1) ^ r),
                (t & 2) | ((f >> 1) & 1),
            )
        )
        for a in range(2)
        for r in range(2)
    ]
    shift = [table(lambda f, t, s=s: (f ^ s, t)) for s in range(fs_size)]

    def send(value, pairs):
        return lax.ppermute(value, ("fs", "tp"), pairs)

    def fast(tokens, norm_gain, gate_weight, up_weight, down_weight, routes, route_logit):
        experts = gate_weight.shape[0]
        fs = lax.axis_index("fs")
        tp = lax.axis_index("tp")
        z1, y, x, c = fs >> 2, fs & 1, tp >> 1, tp & 1
        base = ((fs >> 2) << 2) | (c << 1) | y
        where = jnp.stack([x, z1 ^ x, y, base, tp, fs]).astype(jnp.int32)
        gain_col = norm_gain[:, None]

        floats = tokens.astype(jnp.float32)
        normed = (
            floats * lax.rsqrt(jnp.mean(floats * floats, axis=1, keepdims=True) + EPS)
        ).astype(jnp.bfloat16)
        first_share = jax.nn.sigmoid(route_logit[:, 0] - route_logit[:, 1])
        shares = jnp.stack([first_share, 1.0 - first_share], axis=1)

        picked = []
        for e in range(experts):
            halves = e == 0
            if halves:
                own, leave = cast(gate_weight, up_weight, gain_col, where, e, True)
            else:
                own = leave = cast(gate_weight, up_weight, gain_col, where, e, False)
            got = send(leave, across_x)
            picked.append(pick(where, own, got))
        outs = acc = None
        for e in range(experts):
            halves = e == 0
            here = [send(m, plane[i]) for i, m in enumerate(picked[e])]
            near = [[m] for m in here]
            if halves:
                for i, m in enumerate(here):
                    near[i].append(send(m, across_x))
            far = [[send(m, across_core) for m in item] for item in near]
            pieces = []
            for k in range(fs_size):
                source = far if k & 2 else near
                pieces += source[(k >> 2) * 2 + (k & 1)]
            down = down_weight[e].astype(jnp.bfloat16)
            down_x = send(down, across_x)
            downs = [down, send(down, across_core), down_x, send(down_x, across_core)]
            share = jnp.sum(jnp.where(routes == e, shares, 0.0), axis=1, keepdims=True)
            last = e == experts - 1
            result = expert_step(
                where, share, normed, pieces, downs, outs, acc, e, experts, last, fs_size
            )
            outs, acc = result[:3], result[3]
        mixed = acc
        for s in range(1, fs_size):
            mixed = mixed + send(result[3 + s], shift[s]).astype(jnp.float32)
        return (*outs, mixed.astype(jnp.bfloat16))

    return fast


def shards(tokens, norm_gain, gate_weight, up_weight, down_weight, routes, route_logit):
    gain_col = norm_gain[None, :, None]
    gate_part = (gate_weight * gain_col).astype(jnp.bfloat16)
    up_part = (up_weight * gain_col).astype(jnp.bfloat16)
    down_part = down_weight.astype(jnp.bfloat16)
    gate_one, up_one = (
        lax.all_to_all(gate_part, "tp", split_axis=0, concat_axis=2, tiled=True),
        lax.all_to_all(up_part, "tp", split_axis=0, concat_axis=2, tiled=True),
    )
    gate_mine, up_mine = (
        lax.all_to_all(gate_one, "fs", split_axis=2, concat_axis=1, tiled=True),
        lax.all_to_all(up_one, "fs", split_axis=2, concat_axis=1, tiled=True),
    )
    gate_out, up_out = (
        lax.all_gather(gate_mine, "tp", axis=0, tiled=True),
        lax.all_gather(up_mine, "tp", axis=0, tiled=True),
    )
    down_out = lax.all_gather(down_part, "tp", axis=2, tiled=True)
    total_rows = tokens.shape[0]
    width = tokens.shape[1]
    experts = gate_out.shape[0]
    capacity = total_rows * 5 // 8
    floats = tokens.astype(jnp.float32)
    normed = (floats * lax.rsqrt(jnp.mean(floats * floats, axis=1, keepdims=True) + EPS)).astype(
        jnp.bfloat16
    )
    first_share = jax.nn.sigmoid(route_logit[:, 0] - route_logit[:, 1])
    shares = jnp.stack([first_share, 1.0 - first_share], axis=1)
    chosen = (routes[:, :, None] == jnp.arange(experts, dtype=jnp.int32)[None, None, :]).astype(
        jnp.int32
    )
    counts = jnp.sum(chosen, axis=1)
    before = jnp.cumsum(counts, axis=0) - counts
    slot_index = jnp.sum(chosen * before[:, None, :], axis=2)
    flat_slot = routes * capacity + slot_index
    row_ids = jnp.repeat(jnp.arange(total_rows, dtype=jnp.int32), 2)
    table = (
        jnp.full((experts * capacity,), total_rows, jnp.int32)
        .at[flat_slot.reshape(-1)]
        .set(row_ids)
    )
    gathered = jnp.take(normed, table, axis=0, mode="fill", fill_value=0).reshape(
        experts, capacity, width
    )
    gate_val = jnp.einsum("ecd,edf->ecf", gathered, gate_out, preferred_element_type=jnp.float32)
    up_val = jnp.einsum("ecd,edf->ecf", gathered, up_out, preferred_element_type=jnp.float32)
    hidden = (jax.nn.silu(gate_val) * up_val).astype(jnp.bfloat16)
    results = jnp.einsum("ecf,efd->ecd", hidden, down_out, preferred_element_type=jnp.float32)
    flat_rows = results.reshape(experts * capacity, width)
    first_rows = jnp.take(flat_rows, flat_slot[:, 0], axis=0)
    second_rows = jnp.take(flat_rows, flat_slot[:, 1], axis=0)
    mixed = lax.psum_scatter(
        shares[:, 0:1] * first_rows + shares[:, 1:2] * second_rows,
        "fs",
        scatter_dimension=0,
        tiled=True,
    )
    return (gate_out, up_out, down_out, mixed.astype(jnp.bfloat16))


def solution(mesh):
    fs_size, tp_size = mesh.shape["fs"], mesh.shape["tp"]
    fast = (fs_size, tp_size) == (8, 4)

    def program(*args):
        if not fast:
            return shards(*args)
        return make_fast(fs_size, tp_size)(*args)

    return jax.shard_map(
        program,
        mesh=mesh,
        in_specs=(
            P("tp", None),
            P("fs"),
            P(None, "fs", "tp"),
            P(None, "fs", "tp"),
            P(None, "fs", "tp"),
            P("tp", None),
            P("tp", None),
        ),
        out_specs=(
            P(None, None, "fs"),
            P(None, None, "fs"),
            P(None, "fs", None),
            P(("tp", "fs"), None),
        ),
        check_vma=False,
    )
```

```python
import functools

import jax
import jax.numpy as jnp
from jax import lax
from jax.experimental import pallas as pl
from jax.experimental.pallas import tpu as pltpu
from jax.sharding import PartitionSpec as P


EPS = 0.5
SPLIT_QUARTERS = (4, 4, 1, 0)
ANY = pl.BlockSpec(memory_space=pl.ANY)
SMEM = pl.BlockSpec(memory_space=pltpu.SMEM)
VMEM = pl.BlockSpec(memory_space=pltpu.VMEM)


def cast_whole(gate_ref, up_ref, gain_ref, own_ref):
    gain = gain_ref[...]
    own_ref[0, 0] = (gate_ref[0] * gain).astype(jnp.bfloat16)
    own_ref[0, 1] = (up_ref[0] * gain).astype(jnp.bfloat16)


def cast_halves(where_ref, gate_ref, up_ref, gain_ref, keep_ref, send_ref, *, fixed, half):
    x = where_ref[0]
    for out_ref, at in ((keep_ref, x), (send_ref, 1 - x)):
        split = pl.ds(pl.multiple_of(fixed + at * half, 16), half)
        spans = [(split, pl.ds(fixed, half))]
        if fixed:
            spans.append((pl.ds(0, fixed), pl.ds(0, fixed)))
        for rows, to in spans:
            gain = gain_ref[rows, :]
            out_ref[0, 0, to, :] = (gate_ref[0, rows, :] * gain).astype(jnp.bfloat16)
            out_ref[0, 1, to, :] = (up_ref[0, rows, :] * gain).astype(jnp.bfloat16)


def rows_of(rows, expert):
    quarters = SPLIT_QUARTERS[expert] if expert < len(SPLIT_QUARTERS) else 0
    half = rows * quarters // 8
    return rows - 2 * half, half


def cast(gate_weight, up_weight, gain_col, where, expert):
    _, rows, cols = gate_weight.shape
    wide = cols // 2
    fixed, half = rows_of(rows, expert)
    weight_spec = pl.BlockSpec((1, rows, wide), lambda i: (expert, 0, i))
    gain_spec = pl.BlockSpec((rows, 1), lambda i: (0, 0))
    out_spec = pl.BlockSpec((1, 2, fixed + half, wide), lambda i: (i, 0, 0, 0))
    out = jax.ShapeDtypeStruct((2, 2, fixed + half, wide), jnp.bfloat16)
    if not half:
        whole = pl.pallas_call(
            cast_whole,
            grid=(2,),
            in_specs=[weight_spec, weight_spec, gain_spec],
            out_specs=out_spec,
            out_shape=out,
        )(gate_weight, up_weight, gain_col)
        return whole, whole
    return pl.pallas_call(
        functools.partial(cast_halves, fixed=fixed, half=half),
        grid=(2,),
        in_specs=[SMEM, weight_spec, weight_spec, gain_spec],
        out_specs=[out_spec, out_spec],
        out_shape=[out, out],
    )(where, gate_weight, up_weight, gain_col)


def pick_kernel(where_ref, own_ref, got_ref, *outs):
    flag, y = where_ref[1], where_ref[2]
    for r in range(2):
        at = y if r == 0 else 1 - y

        @pl.when(flag == 0)
        def _():
            outs[r][...] = own_ref[at]
            outs[2 + r][...] = got_ref[at]

        @pl.when(flag != 0)
        def _():
            outs[r][...] = got_ref[at]
            outs[2 + r][...] = own_ref[at]


def pick(where, own, got):
    sides, kinds, rows, wide = own.shape
    block = 128 if rows % 128 == 0 else rows // 2
    in_spec = pl.BlockSpec((sides, 1, block, wide), lambda i, j: (0, i, j, 0))
    out_spec = pl.BlockSpec((1, block, wide), lambda i, j: (i, j, 0))
    out = jax.ShapeDtypeStruct(own.shape[1:], own.dtype)
    return pl.pallas_call(
        pick_kernel,
        grid=(kinds, rows // block),
        in_specs=[SMEM, in_spec, in_spec],
        out_specs=[out_spec] * 4,
        out_shape=[out] * 4,
    )(where, own, got)


def hidden_part(where_ref, normed_ref, pieces, outs, hidden_ref, scratch, expert, spans):
    gate_v, up_v, in_sem, out_sem = scratch
    base, x = where_ref[3], where_ref[0]
    steps = in_sem.shape[2]
    step = gate_v.shape[1] // steps
    fixed, half = spans
    moves = []
    for k in range(8):
        row = (base ^ k) * (fixed + 2 * half)
        if half:
            mine, other = pieces[2 * k], pieces[2 * k + 1]
            moves.append((mine, fixed, half, row + fixed + x * half))
            moves.append((other, 0, half, row + fixed + (1 - x) * half))
        else:
            mine = pieces[k]
        if fixed:
            moves.append((mine, 0, fixed, row))

    def at(n):
        return pl.ds(pl.multiple_of(n * step, step), step)

    def loads(n):
        cols = at(n)
        out = []
        for i, (piece, start, size, row) in enumerate(moves):
            rows = pl.ds(pl.multiple_of(row, 16), size)
            for kind, to in ((0, gate_v), (1, up_v)):
                out.append(
                    pltpu.make_async_copy(
                        piece.at[kind, pl.ds(start, size), cols],
                        to.at[rows, cols],
                        in_sem.at[kind, i, n],
                    )
                )
        return out

    def leaves(n):
        cols = at(n)
        return [
            pltpu.make_async_copy(held.at[:, cols], out.at[expert, :, cols], out_sem.at[kind, n])
            for kind, held, out in ((0, gate_v, outs[0]), (1, up_v, outs[1]))
        ]

    def begin(n, _):
        for item in loads(n):
            item.start()
        return 0

    def compute(n, _):
        for item in loads(n):
            item.wait()
        for item in leaves(n):
            item.start()
        cols = at(n)
        gate_val = jnp.dot(normed_ref[...], gate_v[:, cols], preferred_element_type=jnp.float32)
        up_val = jnp.dot(normed_ref[...], up_v[:, cols], preferred_element_type=jnp.float32)
        hidden_ref[:, cols] = (gate_val / (1.0 + jnp.exp(-gate_val)) * up_val).astype(
            jnp.bfloat16
        )
        return 0

    def end(n, _):
        for item in leaves(n):
            item.wait()
        return 0

    return [functools.partial(lax.fori_loop, 0, steps, f, 0) for f in (begin, compute, end)]


def hidden_scratch(width, units, spans):
    fixed, half = spans
    moves = 8 * ((fixed > 0) + 2 * (half > 0))
    steps = 2 if half else 4
    return [
        pltpu.VMEM((width, units), jnp.bfloat16),
        pltpu.VMEM((width, units), jnp.bfloat16),
        pltpu.SemaphoreType.DMA((2, moves, steps)),
        pltpu.SemaphoreType.DMA((2, steps)),
    ]


def hidden_kernel(where_ref, normed_ref, *refs, expert, pieces_n, spans, joined):
    pieces, refs = refs[:pieces_n], refs[pieces_n:]
    refs = refs[2:] if joined else refs
    for run in hidden_part(
        where_ref, normed_ref, pieces, refs[:2], refs[2], refs[3:], expert, spans
    ):
        run()


def hidden_step(where, normed, pieces, spans, outs, expert, experts):
    tokens, width = normed.shape
    units = pieces[0].shape[2]
    operands = [where, normed, *pieces]
    specs = [SMEM, VMEM] + [ANY] * len(pieces)
    aliases = {}
    if outs is not None:
        aliases = {len(operands): 0, len(operands) + 1: 1}
        operands += list(outs)
        specs += [ANY] * 2
    weight = jax.ShapeDtypeStruct((experts, width, units), jnp.bfloat16)
    body = functools.partial(
        hidden_kernel,
        expert=expert,
        pieces_n=len(pieces),
        spans=spans,
        joined=outs is not None,
    )
    return pl.pallas_call(
        body,
        in_specs=specs,
        out_specs=[ANY, ANY, VMEM],
        out_shape=[weight, weight, jax.ShapeDtypeStruct((tokens, units), jnp.bfloat16)],
        input_output_aliases=aliases,
        scratch_shapes=hidden_scratch(width, units, spans),
        compiler_params=pltpu.CompilerParams(vmem_limit_bytes=48 * 1024 * 1024),
        cost_estimate=pl.CostEstimate(
            flops=4 * tokens * width * units,
            transcendentals=tokens * units,
            bytes_accessed=8 * width * units,
        ),
    )(*operands)


def down_part(where_ref, shares, hiddens, downs, down_out, acc_in, scratch, sources, side):
    down_v, acc_v, down_sem, out_sem, acc_sem = scratch
    tp = where_ref[4]
    count = len(sources)
    wide = downs[0].shape[2]
    places, copies, leaves = [], [], []
    for i in range(2):
        t = tp ^ (2 * side + i)
        cols = pl.ds(pl.multiple_of(t * wide, wide), wide)
        here = pl.ds(pl.multiple_of((t & 1) * wide, wide), wide)
        places.append(here)
        for n, (expert, at) in enumerate(sources):
            copies.append(
                pltpu.make_async_copy(
                    downs[i].at[at[i]], down_v.at[n, :, here], down_sem.at[n, i]
                )
            )
            leaves.append(
                pltpu.make_async_copy(
                    down_v.at[n, :, here], down_out.at[expert, :, cols], out_sem.at[n, i]
                )
            )
    if acc_in is not None:
        acc_copy = pltpu.make_async_copy(acc_in, acc_v, acc_sem.at[0])

    def begin():
        for item in copies:
            item.start()
        if acc_in is not None:
            acc_copy.start()

    def compute():
        for i in range(2):
            for n in range(count):
                copies[i * count + n].wait()
                leaves[i * count + n].start()
                if acc_in is not None and i == 0 and n == 0:
                    acc_copy.wait()
                result = shares[n][...] * jnp.dot(
                    hiddens[n][...], down_v[n, :, places[i]], preferred_element_type=jnp.float32
                )
                fresh = n == 0 and acc_in is None
                acc_v[:, places[i]] = result if fresh else acc_v[:, places[i]] + result

    def end():
        for item in leaves:
            item.wait()

    return begin, compute, end


def down_scratch(count, tokens, fan, wide):
    return [
        pltpu.VMEM((count, fan, 2 * wide), jnp.bfloat16),
        pltpu.VMEM((tokens, 2 * wide), jnp.float32),
        pltpu.SemaphoreType.DMA((count, 2)),
        pltpu.SemaphoreType.DMA((count, 2)),
        pltpu.SemaphoreType.DMA((1,)),
    ]


def down_first_kernel(where_ref, *refs, sources, side, joined):
    count = len(sources)
    shares, hiddens, refs = refs[:count], refs[count : 2 * count], refs[2 * count :]
    downs, refs = refs[:2], refs[2:]
    refs = refs[1:] if joined else refs
    down_out, acc_out, scratch = refs[0], refs[1], refs[2:]
    begin, compute, end = down_part(
        where_ref, shares, hiddens, downs, down_out, None, scratch, sources, side
    )
    begin()
    compute()
    acc_copy = pltpu.make_async_copy(scratch[1], acc_out, scratch[4].at[0])
    acc_copy.start()
    acc_copy.wait()
    end()


def down_first(where, shares, hiddens, downs, sources, outs, experts, side):
    tokens, units = hiddens[0].shape
    _, fan, wide = downs[0].shape
    count = len(sources)
    operands = [where, *shares, *hiddens, *downs]
    specs = [SMEM] + [VMEM] * (2 * count) + [ANY] * 2
    aliases = {}
    if outs is not None:
        aliases = {len(operands): 0}
        operands.append(outs)
        specs.append(ANY)
    return pl.pallas_call(
        functools.partial(
            down_first_kernel, sources=sources, side=side, joined=outs is not None
        ),
        in_specs=specs,
        out_specs=[ANY, ANY],
        out_shape=[
            jax.ShapeDtypeStruct((experts, fan, 4 * wide), jnp.bfloat16),
            jax.ShapeDtypeStruct((tokens, 2 * wide), jnp.float32),
        ],
        input_output_aliases=aliases,
        scratch_shapes=down_scratch(count, tokens, fan, wide),
        compiler_params=pltpu.CompilerParams(vmem_limit_bytes=40 * 1024 * 1024),
        cost_estimate=pl.CostEstimate(
            flops=4 * count * tokens * wide * units,
            transcendentals=0,
            bytes_accessed=8 * count * wide * units,
        ),
    )(*operands)


def hand_out(where_ref, acc_v, own_ref, nears, leave_ref, keep_ref):
    fs = where_ref[5]
    block = own_ref.shape[0]

    def part(s):
        return acc_v[pl.ds(pl.multiple_of((fs ^ s) * block, block), block), :]

    leave_ref[0] = part(5).astype(leave_ref.dtype)
    leave_ref[1] = part(7).astype(leave_ref.dtype)
    keep_ref[0] = part(4)
    keep_ref[1] = part(6)
    own_ref[...] = part(0)
    for s in range(1, 4):
        nears[s - 1][...] = part(s).astype(jnp.bfloat16)


def last_kernel(
    where_ref, normed_ref, share_a, share_b, before_ref, *refs, expert, pieces_n, spans, sources
):
    pieces, refs = refs[:pieces_n], refs[pieces_n:]
    downs, acc_in, refs = refs[2:4], refs[5], refs[6:]
    weights, hidden_ref, down_out, refs = refs[:2], refs[2], refs[3], refs[4:]
    (own_ref, near_1, near_2, near_3, leave_ref, keep_ref), refs = refs[:6], refs[6:]
    begin, compute, end = hidden_part(
        where_ref, normed_ref, pieces, weights, hidden_ref, refs[:4], expert, spans
    )
    down_begin, down_compute, down_end = down_part(
        where_ref,
        [share_a, share_b],
        [before_ref, hidden_ref],
        downs,
        down_out,
        acc_in,
        refs[4:],
        sources,
        0,
    )
    begin()
    down_begin()
    compute()
    down_compute()
    hand_out(where_ref, refs[5], own_ref, (near_1, near_2, near_3), leave_ref, keep_ref)
    end()
    down_end()


def parts_of(block, wide):
    def shape(*dims, dtype=jnp.bfloat16):
        return jax.ShapeDtypeStruct(dims, dtype)

    return [
        shape(2, block, wide),
        shape(2, block, wide, dtype=jnp.float32),
        shape(block, wide, dtype=jnp.float32),
    ]


def last_step(
    where, normed, shares, before, pieces, spans, weights, downs, down_out, acc, experts, parts
):
    tokens, width = normed.shape
    units = pieces[0].shape[2]
    _, fan, wide = downs[0].shape
    expert = experts - 1
    count = len(pieces)
    leave, keep, own = parts_of(tokens // parts, 2 * wide)
    near = jax.ShapeDtypeStruct(own.shape, jnp.bfloat16)
    weight = jax.ShapeDtypeStruct((experts, width, units), jnp.bfloat16)
    sources = tuple((e, (e, e)) for e in (expert - 1, expert))
    return pl.pallas_call(
        functools.partial(
            last_kernel, expert=expert, pieces_n=count, spans=spans, sources=sources
        ),
        in_specs=[SMEM] + [VMEM] * 4 + [ANY] * (count + 6),
        out_specs=[ANY, ANY, VMEM, ANY] + [VMEM] * 6,
        out_shape=[
            weight,
            weight,
            jax.ShapeDtypeStruct((tokens, units), jnp.bfloat16),
            jax.ShapeDtypeStruct(down_out.shape, jnp.bfloat16),
            own,
            near,
            near,
            near,
            leave,
            keep,
        ],
        input_output_aliases={5 + count: 0, 6 + count: 1, 9 + count: 3},
        scratch_shapes=hidden_scratch(width, units, spans)
        + down_scratch(2, tokens, fan, wide),
        compiler_params=pltpu.CompilerParams(vmem_limit_bytes=50 * 1024 * 1024),
        cost_estimate=pl.CostEstimate(
            flops=6 * tokens * width * units,
            transcendentals=tokens * units,
            bytes_accessed=8 * width * units,
        ),
        name="last_0",
    )(where, normed, *shares, before, *pieces, *weights, *downs, down_out, acc)


def rest_kernel(where_ref, share_a, share_b, hidden_a, hidden_b, *refs, sources):
    nears_a, downs, acc_in = refs[:3], refs[3:5], refs[6]
    down_out, own_ref, near_1, near_2, near_3, leave_ref, keep_ref = refs[7:14]
    scratch = refs[14:]
    begin, compute, end = down_part(
        where_ref,
        [share_a, share_b],
        [hidden_a, hidden_b],
        downs,
        down_out,
        acc_in,
        scratch,
        sources,
        1,
    )
    begin()
    nears = (near_1, near_2, near_3)
    for i in range(3):
        nears[i][0] = nears_a[i][...]
    compute()
    hand_out(
        where_ref, scratch[1], own_ref, [ref.at[1] for ref in nears], leave_ref, keep_ref
    )
    end()


def rest_step(where, shares, hiddens, nears, downs, down_out, acc, experts, parts):
    tokens, units = hiddens[0].shape
    _, fan, wide = downs[0].shape
    leave, keep, own = parts_of(tokens // parts, 2 * wide)
    sources = ((experts - 2, (0, 0)), (experts - 1, (1, 1)))
    return pl.pallas_call(
        functools.partial(rest_kernel, sources=sources),
        in_specs=[SMEM] + [VMEM] * 7 + [ANY] * 4,
        out_specs=[ANY] + [VMEM] * 6,
        out_shape=[jax.ShapeDtypeStruct(down_out.shape, jnp.bfloat16), own]
        + [jax.ShapeDtypeStruct(leave.shape, jnp.bfloat16)] * 3
        + [leave, keep],
        input_output_aliases={10: 0},
        scratch_shapes=down_scratch(2, tokens, fan, wide),
        compiler_params=pltpu.CompilerParams(vmem_limit_bytes=40 * 1024 * 1024),
        cost_estimate=pl.CostEstimate(
            flops=8 * tokens * wide * units, transcendentals=0, bytes_accessed=16 * wide * units
        ),
        name="last_1",
    )(where, *shares, *hiddens, *nears, *downs, down_out, acc)


def total_kernel(keep_ref, got_ref, *outs):
    for i in range(2):
        total = keep_ref[i] + got_ref[i].astype(jnp.float32)
        outs[i][...] = total.astype(outs[i].dtype)


def total_step(keep, got):
    out = jax.ShapeDtypeStruct(got.shape[1:], got.dtype)
    return pl.pallas_call(
        total_kernel, in_specs=[VMEM, VMEM], out_specs=[VMEM, VMEM], out_shape=[out, out]
    )(keep, got)


def make_fast(fs_size, tp_size):
    def table(target):
        pairs = []
        for f in range(fs_size):
            for t in range(tp_size):
                to_f, to_t = target(f, t)
                pairs.append((f * tp_size + t, to_f * tp_size + to_t))
        return pairs

    across_x = table(lambda f, t: (f, t ^ 2))
    across_core = table(lambda f, t: (f, t ^ 1))
    plane = [
        table(
            lambda f, t, a=a, r=r: (
                ((f >> 2) ^ a) << 2 | (t & 1) << 1 | ((f & 1) ^ r),
                (t & 2) | ((f >> 1) & 1),
            )
        )
        for a in range(2)
        for r in range(2)
    ]
    shift = [table(lambda f, t, s=s: (f ^ s, t)) for s in range(fs_size)]

    def send(value, pairs):
        return lax.ppermute(value, ("fs", "tp"), pairs)

    def fast(tokens, norm_gain, gate_weight, up_weight, down_weight, routes, route_logit):
        experts = gate_weight.shape[0]
        fs = lax.axis_index("fs")
        tp = lax.axis_index("tp")
        z1, y, x, c = fs >> 2, fs & 1, tp >> 1, tp & 1
        base = ((fs >> 2) << 2) | (c << 1) | y
        where = jnp.stack([x, z1 ^ x, y, base, tp, fs]).astype(jnp.int32)
        gain_col = norm_gain[:, None]

        floats = tokens.astype(jnp.float32)
        normed = (
            floats * lax.rsqrt(jnp.mean(floats * floats, axis=1, keepdims=True) + EPS)
        ).astype(jnp.bfloat16)
        first_share = jax.nn.sigmoid(route_logit[:, 0] - route_logit[:, 1])
        shares = jnp.stack([first_share, 1.0 - first_share], axis=1)

        picked = []
        for e in range(experts):
            own, leave = cast(gate_weight, up_weight, gain_col, where, e)
            got = send(leave, across_x)
            picked.append(pick(where, own, got))
        early, final = experts - 2, experts - 1
        down = down_weight.astype(jnp.bfloat16)
        down_x = [send(down[:early], across_x), send(down[early:], across_x)]
        down_c = send(down, across_core)
        down_y = [send(down_x[0], across_core), send(down_x[1], across_core)]
        shares = [
            jnp.sum(jnp.where(routes == e, shares, 0.0), axis=1, keepdims=True)
            for e in range(experts)
        ]
        outs = None
        hiddens = []
        for e in range(experts):
            spans = rows_of(gate_weight.shape[1], e)
            fixed, half = spans
            here = [send(m, plane[i]) for i, m in enumerate(picked[e])]
            near = [[m] for m in here]
            if half and fixed:
                gated = lax.optimization_barrier((*here, hiddens[-1]))[:-1]
                for i, m in enumerate(gated):
                    near[i].append(send(m[:, fixed:], across_x))
            elif half:
                for i, m in enumerate(here):
                    near[i].append(send(m[:, fixed:], across_x))
            far = [[send(m, across_core) for m in item] for item in near]
            pieces = []
            for k in range(fs_size):
                source = far if k & 2 else near
                pieces += source[(k >> 2) * 2 + (k & 1)]
            if e < final:
                *outs, hidden = hidden_step(where, normed, pieces, spans, outs, e, experts)
                hiddens.append(hidden)
        down_out, accs = None, []
        for side in range(2):
            down_out, acc = down_first(
                where,
                shares[:early],
                hiddens[:early],
                [down_x[0], down_y[0]] if side else [down, down_c],
                tuple((e, (e, e)) for e in range(early)),
                down_out,
                experts,
                side,
            )
            accs.append(acc)
        *outs, hidden, down_out, own_a, near_1, near_2, near_3, leave_a, keep_a = last_step(
            where, normed, shares[early:], hiddens[early], pieces, spans, outs, [down, down_c],
            down_out, accs[0], experts, fs_size,
        )
        down_out, own_b, *nears, leave_b, keep_b = rest_step(
            where, shares[early:], [hiddens[early], hidden], [near_1, near_2, near_3],
            [down_x[1], down_y[1]], down_out, accs[1], experts, fs_size,
        )
        nears = [send(item, shift[s + 1]) for s, item in enumerate(nears)]
        sums = []
        for side, (own, leave, keep) in enumerate(
            ((own_a, leave_a, keep_a), (own_b, leave_b, keep_b))
        ):
            total = total_step(keep, send(leave, shift[1]))
            far = [send(total[i], shift[4 + 2 * i]) for i in range(2)]
            for item in [near[side] for near in nears] + far:
                own = own + item.astype(jnp.float32)
            sums.append(own.astype(jnp.bfloat16))
        mixed = jnp.where(
            x == 0, jnp.concatenate(sums, axis=1), jnp.concatenate(sums[::-1], axis=1)
        )
        return (*outs, down_out, mixed)

    return fast


def shards(tokens, norm_gain, gate_weight, up_weight, down_weight, routes, route_logit):
    gain_col = norm_gain[None, :, None]
    gate_part = (gate_weight * gain_col).astype(jnp.bfloat16)
    up_part = (up_weight * gain_col).astype(jnp.bfloat16)
    down_part = down_weight.astype(jnp.bfloat16)
    gate_one, up_one = (
        lax.all_to_all(gate_part, "tp", split_axis=0, concat_axis=2, tiled=True),
        lax.all_to_all(up_part, "tp", split_axis=0, concat_axis=2, tiled=True),
    )
    gate_mine, up_mine = (
        lax.all_to_all(gate_one, "fs", split_axis=2, concat_axis=1, tiled=True),
        lax.all_to_all(up_one, "fs", split_axis=2, concat_axis=1, tiled=True),
    )
    gate_out, up_out = (
        lax.all_gather(gate_mine, "tp", axis=0, tiled=True),
        lax.all_gather(up_mine, "tp", axis=0, tiled=True),
    )
    down_out = lax.all_gather(down_part, "tp", axis=2, tiled=True)
    total_rows = tokens.shape[0]
    width = tokens.shape[1]
    experts = gate_out.shape[0]
    capacity = total_rows * 5 // 8
    floats = tokens.astype(jnp.float32)
    normed = (floats * lax.rsqrt(jnp.mean(floats * floats, axis=1, keepdims=True) + EPS)).astype(
        jnp.bfloat16
    )
    first_share = jax.nn.sigmoid(route_logit[:, 0] - route_logit[:, 1])
    shares = jnp.stack([first_share, 1.0 - first_share], axis=1)
    chosen = (routes[:, :, None] == jnp.arange(experts, dtype=jnp.int32)[None, None, :]).astype(
        jnp.int32
    )
    counts = jnp.sum(chosen, axis=1)
    before = jnp.cumsum(counts, axis=0) - counts
    slot_index = jnp.sum(chosen * before[:, None, :], axis=2)
    flat_slot = routes * capacity + slot_index
    row_ids = jnp.repeat(jnp.arange(total_rows, dtype=jnp.int32), 2)
    table = (
        jnp.full((experts * capacity,), total_rows, jnp.int32)
        .at[flat_slot.reshape(-1)]
        .set(row_ids)
    )
    gathered = jnp.take(normed, table, axis=0, mode="fill", fill_value=0).reshape(
        experts, capacity, width
    )
    gate_val = jnp.einsum("ecd,edf->ecf", gathered, gate_out, preferred_element_type=jnp.float32)
    up_val = jnp.einsum("ecd,edf->ecf", gathered, up_out, preferred_element_type=jnp.float32)
    hidden = (jax.nn.silu(gate_val) * up_val).astype(jnp.bfloat16)
    results = jnp.einsum("ecf,efd->ecd", hidden, down_out, preferred_element_type=jnp.float32)
    flat_rows = results.reshape(experts * capacity, width)
    first_rows = jnp.take(flat_rows, flat_slot[:, 0], axis=0)
    second_rows = jnp.take(flat_rows, flat_slot[:, 1], axis=0)
    mixed = lax.psum_scatter(
        shares[:, 0:1] * first_rows + shares[:, 1:2] * second_rows,
        "fs",
        scatter_dimension=0,
        tiled=True,
    )
    return (gate_out, up_out, down_out, mixed.astype(jnp.bfloat16))


def solution(mesh):
    fs_size, tp_size = mesh.shape["fs"], mesh.shape["tp"]
    fast = (fs_size, tp_size) == (8, 4)

    def program(*args):
        if not fast:
            return shards(*args)
        return make_fast(fs_size, tp_size)(*args)

    return jax.shard_map(
        program,
        mesh=mesh,
        in_specs=(
            P("tp", None),
            P("fs"),
            P(None, "fs", "tp"),
            P(None, "fs", "tp"),
            P(None, "fs", "tp"),
            P("tp", None),
            P("tp", None),
        ),
        out_specs=(
            P(None, None, "fs"),
            P(None, None, "fs"),
            P(None, "fs", None),
            P(("tp", "fs"), None),
        ),
        check_vma=False,
    )
```
